32 devices in a mesh: fs: 32 (over z, y, x, core), tp: 1.
Axes of the slice: x: 2, y: 2, z: 4, core: 2. Of those that a mesh axis runs over, the one named last changes fastest.
Arguments:
- later_input: bfloat16 [6144, 2048], P(('fs', 'tp')), may hold values from -6 to 6
- earlier_input: bfloat16 [6144, 2048], P(('fs', 'tp')), may hold values from -6 to 6
- cotangent: bfloat16 [6144, 2048], P(('fs', 'tp')), may hold values from -6 to 6
- gate_weight: bfloat16 [2048, 3072], P('fs', 'tp'), may hold values from -0.125 to 0.125
- up_weight: bfloat16 [2048, 3072], P('fs', 'tp'), may hold values from -0.125 to 0.125
- down_weight: bfloat16 [2048, 3072], P('fs', 'tp'), may hold values from -0.109375 to 0.109375
- down_grad_sum: float32 [2048, 3072], P('fs', 'tp'), may hold values from -6 to 6
Outputs:
- later_output: bfloat16 [6144, 2048], P(('fs', 'tp'))
- earlier_grad_input: bfloat16 [6144, 2048], P(('fs', 'tp'))
- new_down_grad_sum: float32 [2048, 3072], P('fs', 'tp')
The draws below stay inside these ranges and needn't reach their ends.
All inputs are finite; a program needn't handle non-finite values.
Results may differ from the reference program's by a relative error of at most 0.0057.
Values may be sent and summed in bfloat16 or wider, within the bound.
A program may use at most 192 MiB of HBM per device.

```python
import jax
import jax.numpy as jnp
from jax import lax

D = 2048
FF = 3072
TOKENS = 6144
N_TP = 1


def raised(result, key, source, target, blocks, factor):
    owner, partner = [(jnp.arange(result.shape[axis_at]) // (result.shape[axis_at] // blocks)).reshape([-1 if axis == axis_at else 1 for axis in range(result.ndim)]) for axis_at in (source, target)]
    chosen = jax.random.permutation(key, blocks)[partner]
    strong = (owner == chosen) | (owner == (partner + blocks // 2) % blocks)
    return jnp.where(strong, factor * result, result)


def block_scale(rng, shape, split, low, top_value):
    factor_of, own = 1.0, jax.random.fold_in(rng, 6)
    for position, parts in split:
        heights = jnp.exp(jax.random.uniform(jax.random.fold_in(own, position), (parts,), jnp.float32, low / len(split), top_value / len(split)))
        factor_of = factor_of * jnp.repeat(heights, shape[position] // parts).reshape([-1 if axis == position else 1 for axis in range(len(shape))])
    return factor_of


def noise(stream_key, dims, deviation, most, shards=(), kind=jnp.bfloat16):
    loudness = block_scale(stream_key, dims, shards, -0.22, 0.18) if shards else 1.0
    entries = jax.random.normal(stream_key, dims, jnp.float32) * deviation * loudness
    return jnp.minimum(jnp.maximum(entries, -most), most).astype(kind)


def bell_draw_with(own_key, dims, deviation, most, split, heavy, held_as=jnp.bfloat16):
    entries = deviation * jax.random.normal(own_key, dims, jnp.float32)
    if split:
        entries = entries * block_scale(own_key, dims, split, -0.22, 0.18)
    return jnp.clip(raised(entries, jax.random.fold_in(own_key, 3), *heavy), -most, most).astype(held_as)


def setup_inputs(seed: int = 0) -> dict:
    keys = jax.random.split(jax.random.key(seed), 8)
    later_input = noise(keys[0], (TOKENS, D), 1.0, 6.0, ((0, 32),))
    earlier_input = noise(keys[1], (TOKENS, D), 1.0, 6.0, ((0, 32),))
    cotangent = bell_draw_with(keys[2], (TOKENS, D), 1.0, 6.0, ((0, 32),), (0, 1, 32, 2.75))
    gate_weight = noise(keys[3], (D, FF), D ** -0.5, 0.125, ((0, 32),))
    up_weight = noise(keys[4], (D, FF), D ** -0.5, 0.125, ((0, 32),))
    down_weight = noise(keys[5], (D, FF), FF ** -0.5, 0.109375, ((0, 32),))
    down_grad_sum = noise(keys[6], (D, FF), 1.0, 6.0, ((0, 32),), jnp.float32)
    return dict(later_input=later_input, earlier_input=earlier_input, cotangent=cotangent, gate_weight=gate_weight, up_weight=up_weight, down_weight=down_weight, down_grad_sum=down_grad_sum)


def partial_rows(gradients, weights, first_unit, last_unit):
    return jnp.dot(gradients[:, first_unit:last_unit], weights[:, first_unit:last_unit].T, preferred_element_type=jnp.float32)


def rounded_sum(total, partial_value):
    kept = lax.optimization_barrier(partial_value.astype(jnp.bfloat16))
    return total + kept.astype(jnp.float32)


def reference(later_input, earlier_input, cotangent, gate_weight, up_weight, down_weight, down_grad_sum):
    block_width = FF // N_TP
    gate_later = jnp.dot(later_input, gate_weight, preferred_element_type=jnp.float32)
    up_later = jnp.dot(later_input, up_weight, preferred_element_type=jnp.float32)
    hidden_later = (jax.nn.silu(gate_later) * up_later).astype(jnp.bfloat16)
    output_total = jnp.zeros((TOKENS, D), jnp.float32)
    for block_index in range(N_TP):
        first_unit = block_index * block_width
        partial_value = partial_rows(hidden_later, down_weight, first_unit, first_unit + block_width)
        output_total = rounded_sum(output_total, partial_value)
    later_output = output_total.astype(jnp.bfloat16)

    gate_early = jnp.dot(earlier_input, gate_weight, preferred_element_type=jnp.float32)
    up_early = jnp.dot(earlier_input, up_weight, preferred_element_type=jnp.float32)
    sigmoid_gate = jax.nn.sigmoid(gate_early)
    activated = gate_early * sigmoid_gate
    hidden_early = (activated * up_early).astype(jnp.bfloat16)
    grad_hidden = jnp.dot(cotangent, down_weight, preferred_element_type=jnp.float32)
    grad_gate = (grad_hidden * up_early * sigmoid_gate * (1.0 + gate_early * (1.0 - sigmoid_gate))).astype(jnp.bfloat16)
    grad_up = (grad_hidden * activated).astype(jnp.bfloat16)
    input_total = jnp.zeros((TOKENS, D), jnp.float32)
    for block_index in range(N_TP):
        first_unit = block_index * block_width
        last_unit = first_unit + block_width
        partial_value = partial_rows(grad_gate, gate_weight, first_unit, last_unit) + partial_rows(grad_up, up_weight, first_unit, last_unit)
        input_total = rounded_sum(input_total, partial_value)
    earlier_grad_input = input_total.astype(jnp.bfloat16)

    weight_grad = jnp.dot(cotangent.T, hidden_early, preferred_element_type=jnp.float32)
    new_down_grad_sum = down_grad_sum + weight_grad * (TOKENS ** -0.5)
    return (later_output, earlier_grad_input, new_down_grad_sum)
```

```python
import jax
import jax.numpy as jnp
from jax import lax
from jax.sharding import PartitionSpec as P

QUAD = 4


def contract_last(leading, trailing):
    return lax.dot_general(
        leading, trailing, (((1,), (1,)), ((), ())), preferred_element_type=jnp.float32
    )


def add_parts(received, group):
    pieces = received.reshape(group, received.shape[0] // group, received.shape[1])
    return jnp.sum(pieces.astype(jnp.float32), axis=0).astype(jnp.bfloat16)


def shards(
    later_input, earlier_input, cotangent, gate_weight, up_weight, down_weight, down_grad_sum
):
    group = lax.axis_size("tp")
    later_rows, early_rows, grad_rows = (
        lax.all_gather(later_input, "tp", axis=0, tiled=True),
        lax.all_gather(earlier_input, "tp", axis=0, tiled=True),
        lax.all_gather(cotangent, "tp", axis=0, tiled=True),
    )
    columns = later_rows
    gate_later = jnp.dot(
        columns,
        lax.all_gather(gate_weight, "fs", axis=0, tiled=True),
        preferred_element_type=jnp.float32,
    )
    up_later = jnp.dot(
        columns,
        lax.all_gather(up_weight, "fs", axis=0, tiled=True),
        preferred_element_type=jnp.float32,
    )
    hidden_later = (jax.nn.silu(gate_later) * up_later).astype(jnp.bfloat16)
    partials = contract_last(hidden_later, lax.all_gather(down_weight, "fs", axis=0, tiled=True))
    gate_whole, up_whole, down_whole = (
        lax.all_gather(gate_weight, "fs", axis=0, tiled=True),
        lax.all_gather(up_weight, "fs", axis=0, tiled=True),
        lax.all_gather(down_weight, "fs", axis=0, tiled=True),
    )
    output_received = lax.all_to_all(
        partials.astype(jnp.bfloat16), "tp", split_axis=0, concat_axis=0, tiled=True
    )
    later_output = add_parts(output_received, group)
    gate_early = jnp.dot(early_rows, gate_whole, preferred_element_type=jnp.float32)
    up_early = jnp.dot(early_rows, up_whole, preferred_element_type=jnp.float32)
    sigmoid_gate = jax.nn.sigmoid(gate_early)
    activated = gate_early * sigmoid_gate
    hidden_early = (activated * up_early).astype(jnp.bfloat16)
    grad_hidden = jnp.dot(grad_rows, down_whole, preferred_element_type=jnp.float32)
    grad_gate = (
        grad_hidden * up_early * sigmoid_gate * (1.0 + gate_early * (1.0 - sigmoid_gate))
    ).astype(jnp.bfloat16)
    grad_up = (grad_hidden * activated).astype(jnp.bfloat16)
    input_partial = contract_last(grad_gate, gate_whole) + contract_last(grad_up, up_whole)
    input_received = lax.all_to_all(
        input_partial.astype(jnp.bfloat16), "tp", split_axis=0, concat_axis=0, tiled=True
    )
    earlier_grad_input = add_parts(input_received, group)
    columns = grad_rows
    summed = lax.psum_scatter(
        lax.dot_general(
            columns, hidden_early, (((0,), (0,)), ((), ())), preferred_element_type=jnp.float32
        ),
        "fs",
        scatter_dimension=0,
        tiled=True,
    )
    factor = (later_rows.shape[0] * lax.axis_size("fs")) ** (-0.5)
    return (later_output, earlier_grad_input, down_grad_sum + summed * factor)

def quads_of(total):
    return [[first + place for place in range(QUAD)] for first in range(0, total, QUAD)]


def lanes_of(total):
    return [[first + place for first in range(0, total, QUAD)] for place in range(QUAD)]


def swap(value, bit):
    total = lax.axis_size("fs")
    return lax.ppermute(value, "fs", [(index, index ^ bit) for index in range(total)])


def gather_tokens(rows):
    far = swap(rows, 2)
    return jnp.concatenate([rows, swap(rows, 1), far, swap(far, 1)], axis=0)


def return_tokens(partial):
    blocks = partial.astype(jnp.bfloat16).reshape(QUAD, -1, partial.shape[1])
    mine = partial.reshape(blocks.shape)
    near = swap(jnp.stack([blocks[1], blocks[3]]), 1).astype(jnp.float32)
    far = swap((mine[2] + near[1]).astype(jnp.bfloat16), 2)
    return (mine[0] + near[0] + far.astype(jnp.float32)).astype(jnp.bfloat16)


def gather_weight(weight):
    total = lax.axis_size("fs")
    part = lax.all_to_all(
        weight, "fs", split_axis=1, concat_axis=0, tiled=True, axis_index_groups=quads_of(total)
    )
    return lax.all_gather(part, "fs", axis=0, tiled=True, axis_index_groups=lanes_of(total))


def quad_shards(
    later_input, earlier_input, cotangent, gate_weight, up_weight, down_weight, down_grad_sum
):
    total = lax.axis_size("fs")
    gate_whole = gather_weight(gate_weight)
    up_whole = gather_weight(up_weight)
    down_whole = gather_weight(down_weight)
    early_rows = gather_tokens(earlier_input)
    grad_rows = gather_tokens(cotangent)
    later_rows = gather_tokens(later_input)

    gate_early = jnp.dot(early_rows, gate_whole, preferred_element_type=jnp.float32)
    up_early = jnp.dot(early_rows, up_whole, preferred_element_type=jnp.float32)
    sigmoid_gate = jax.nn.sigmoid(gate_early)
    activated = gate_early * sigmoid_gate
    hidden_early = (activated * up_early).astype(jnp.bfloat16)
    partial_sum = lax.dot_general(
        grad_rows, hidden_early, (((0,), (0,)), ((), ())), preferred_element_type=jnp.float32
    ).astype(jnp.bfloat16)
    summed = lax.psum_scatter(
        partial_sum,
        "fs",
        scatter_dimension=0,
        tiled=True,
        axis_index_groups=lanes_of(total),
    )
    gate_later = jnp.dot(later_rows, gate_whole, preferred_element_type=jnp.float32)
    up_later = jnp.dot(later_rows, up_whole, preferred_element_type=jnp.float32)
    hidden_later = (jax.nn.silu(gate_later) * up_later).astype(jnp.bfloat16)

    grad_hidden = jnp.dot(grad_rows, down_whole, preferred_element_type=jnp.float32)
    grad_gate = (
        grad_hidden * up_early * sigmoid_gate * (1.0 + gate_early * (1.0 - sigmoid_gate))
    ).astype(jnp.bfloat16)
    grad_up = (grad_hidden * activated).astype(jnp.bfloat16)
    later_output = return_tokens(contract_last(hidden_later, down_whole))
    earlier_grad_input = return_tokens(
        contract_last(grad_gate, gate_whole) + contract_last(grad_up, up_whole)
    )
    own_rows = lax.all_to_all(
        summed, "fs", split_axis=0, concat_axis=1, tiled=True, axis_index_groups=quads_of(total)
    )
    factor = (later_input.shape[0] * total) ** (-0.5)
    return (
        later_output,
        earlier_grad_input,
        down_grad_sum + own_rows.astype(jnp.float32) * factor,
    )


def solution(mesh):
    in_specs = (
        P(("fs", "tp"), None),
        P(("fs", "tp"), None),
        P(("fs", "tp"), None),
        P("fs", "tp"),
        P("fs", "tp"),
        P("fs", "tp"),
        P("fs", "tp"),
    )
    out_specs = (P(("fs", "tp"), None), P(("fs", "tp"), None), P("fs", "tp"))
    split = mesh.shape["tp"] == 1 and mesh.shape["fs"] % (2 * QUAD) == 0
    body = quad_shards if split else shards
    return jax.shard_map(body, mesh=mesh, in_specs=in_specs, out_specs=out_specs, check_vma=False)
```

```python
import functools

import jax
import jax.numpy as jnp
from jax import lax
from jax.experimental import pallas as pl
from jax.experimental.pallas import tpu as pltpu
from jax.sharding import PartitionSpec as P

QUAD = 4


def contract_last(leading, trailing):
    return lax.dot_general(
        leading, trailing, (((1,), (1,)), ((), ())), preferred_element_type=jnp.float32
    )


def add_parts(received, group):
    pieces = received.reshape(group, received.shape[0] // group, received.shape[1])
    return jnp.sum(pieces.astype(jnp.float32), axis=0).astype(jnp.bfloat16)


def shards(
    later_input, earlier_input, cotangent, gate_weight, up_weight, down_weight, down_grad_sum
):
    group = lax.axis_size("tp")
    later_rows, early_rows, grad_rows = (
        lax.all_gather(later_input, "tp", axis=0, tiled=True),
        lax.all_gather(earlier_input, "tp", axis=0, tiled=True),
        lax.all_gather(cotangent, "tp", axis=0, tiled=True),
    )
    columns = later_rows
    gate_later = jnp.dot(
        columns,
        lax.all_gather(gate_weight, "fs", axis=0, tiled=True),
        preferred_element_type=jnp.float32,
    )
    up_later = jnp.dot(
        columns,
        lax.all_gather(up_weight, "fs", axis=0, tiled=True),
        preferred_element_type=jnp.float32,
    )
    hidden_later = (jax.nn.silu(gate_later) * up_later).astype(jnp.bfloat16)
    partials = contract_last(hidden_later, lax.all_gather(down_weight, "fs", axis=0, tiled=True))
    gate_whole, up_whole, down_whole = (
        lax.all_gather(gate_weight, "fs", axis=0, tiled=True),
        lax.all_gather(up_weight, "fs", axis=0, tiled=True),
        lax.all_gather(down_weight, "fs", axis=0, tiled=True),
    )
    output_received = lax.all_to_all(
        partials.astype(jnp.bfloat16), "tp", split_axis=0, concat_axis=0, tiled=True
    )
    later_output = add_parts(output_received, group)
    gate_early = jnp.dot(early_rows, gate_whole, preferred_element_type=jnp.float32)
    up_early = jnp.dot(early_rows, up_whole, preferred_element_type=jnp.float32)
    sigmoid_gate = jax.nn.sigmoid(gate_early)
    activated = gate_early * sigmoid_gate
    hidden_early = (activated * up_early).astype(jnp.bfloat16)
    grad_hidden = jnp.dot(grad_rows, down_whole, preferred_element_type=jnp.float32)
    grad_gate = (
        grad_hidden * up_early * sigmoid_gate * (1.0 + gate_early * (1.0 - sigmoid_gate))
    ).astype(jnp.bfloat16)
    grad_up = (grad_hidden * activated).astype(jnp.bfloat16)
    input_partial = contract_last(grad_gate, gate_whole) + contract_last(grad_up, up_whole)
    input_received = lax.all_to_all(
        input_partial.astype(jnp.bfloat16), "tp", split_axis=0, concat_axis=0, tiled=True
    )
    earlier_grad_input = add_parts(input_received, group)
    columns = grad_rows
    summed = lax.psum_scatter(
        lax.dot_general(
            columns, hidden_early, (((0,), (0,)), ((), ())), preferred_element_type=jnp.float32
        ),
        "fs",
        scatter_dimension=0,
        tiled=True,
    )
    factor = (later_rows.shape[0] * lax.axis_size("fs")) ** (-0.5)
    return (later_output, earlier_grad_input, down_grad_sum + summed * factor)

def quads_of(total):
    return [[first + place for place in range(QUAD)] for first in range(0, total, QUAD)]


def lanes_of(total):
    return [[first + place for first in range(0, total, QUAD)] for place in range(QUAD)]


def swap(value, bit):
    total = lax.axis_size("fs")
    return lax.ppermute(value, "fs", [(index, index ^ bit) for index in range(total)])


def return_tokens(partial):
    blocks = partial.astype(jnp.bfloat16).reshape(QUAD, -1, partial.shape[1])
    mine = partial.reshape(blocks.shape)
    near = swap(jnp.stack([blocks[1], blocks[3]]), 1).astype(jnp.float32)
    far = swap((mine[2] + near[1]).astype(jnp.bfloat16), 2)
    return (mine[0] + near[0] + far.astype(jnp.float32)).astype(jnp.bfloat16)

def ring_group(place, ring):
    half = lax.div(2 * place, ring)
    return 2 * place * (1 - half) + (2 * (ring - 1 - place) + 1) * half


def ring_place(group, ring):
    odd = lax.rem(group, 2)
    return lax.div(group, 2) * (1 - odd) + (ring - 1 - lax.div(group, 2)) * odd


def gather_kernel(ring, weights, tokens, *refs):
    weight_refs, token_refs = refs[:weights], refs[weights : weights + tokens]
    outs = refs[weights + tokens : 2 * (weights + tokens)]
    whole_refs, rows_refs = outs[:weights], outs[weights:]
    ring_send, ring_recv, quad_send, quad_recv, token_send, token_recv, local_sem = refs[
        2 * (weights + tokens) :
    ]
    me = lax.axis_index("fs")
    group, lane = lax.div(me, QUAD), lax.rem(me, QUAD)
    low, high = lax.rem(lane, 2), lax.div(lane, 2)
    relative = [lane, lane + 1 - 2 * low, lane + 2 - 4 * high, QUAD - 1 - lane]
    peers = [group * QUAD + other for other in relative]
    place = ring_place(group, ring)
    around = [
        ring_group(lax.rem(place + shift, ring), ring) * QUAD + lane for shift in (1, ring - 1)
    ]
    depth = weight_refs[0].shape[0]
    width = weight_refs[0].shape[1] // QUAD

    barrier = pltpu.get_barrier_semaphore()
    for other in peers[1:] + around:
        pl.semaphore_signal(
            barrier, inc=1, device_id={"fs": other}, device_id_type=pl.DeviceIdType.MESH
        )
    pl.semaphore_wait(barrier, QUAD + 1)

    def remote(source, target, send, recv, other):
        return pltpu.make_async_remote_copy(
            src_ref=source,
            dst_ref=target,
            send_sem=send,
            recv_sem=recv,
            device_id={"fs": other},
            device_id_type=pl.DeviceIdType.MESH,
        )

    def slab(weight, owner, member):
        first = pl.multiple_of((owner * QUAD + member) * depth, depth)
        return whole_refs[weight].at[pl.ds(first, depth), :]

    def columns(weight, member):
        return weight_refs[weight].at[:, pl.ds(pl.multiple_of(member * width, width), width)]

    sent, kept = [], []
    quad, hops, rows = {}, {}, {}
    for weight in range(weights):
        for far in (3, 2, 1):
            copy = remote(
                columns(weight, relative[far]),
                slab(weight, group, lane),
                quad_send.at[weight, far - 1],
                quad_recv.at[weight, far - 1],
                peers[far],
            )
            copy.start()
            quad[weight, far] = copy
            sent.append(copy)
    for weight in range(weights):
        copy = pltpu.make_async_copy(
            columns(weight, lane), slab(weight, group, lane), local_sem.at[weight]
        )
        copy.start()
        kept.append(copy)

    def row_block(token, block):
        count = token_refs[token].shape[0]
        return rows_refs[token].at[pl.ds(block * count, count), :]

    def send_rows(token, source, block, slot, other):
        copy = remote(
            source,
            row_block(token, block),
            token_send.at[token, slot],
            token_recv.at[token, slot],
            other,
        )
        copy.start()
        rows[token, slot] = copy
        sent.append(copy)

    for token in range(tokens):
        send_rows(token, token_refs[token], 2, 1, peers[2])
    for token in range(tokens):
        send_rows(token, token_refs[token], 1, 0, peers[1])
        copy = pltpu.make_async_copy(
            token_refs[token], row_block(token, 0), local_sem.at[weights + token]
        )
        copy.start()
        kept.append(copy)

    for step in range(ring - 1):
        for weight in range(weights):
            for piece in (0, 1, 3, 2):
                if step:
                    hops[weight, piece, step - 1].wait_recv()
                elif piece:
                    quad[weight, piece].wait_recv()
                forward = piece in (0, 3)
                back = ring - step if forward else step
                owner = ring_group(lax.rem(place + back, ring), ring)
                target = slab(weight, owner, relative[piece])
                copy = remote(
                    columns(weight, lane) if step == 0 and piece == 0 else target,
                    target,
                    ring_send.at[weight, piece, step],
                    ring_recv.at[weight, piece, step],
                    around[0 if forward else 1],
                )
                copy.start()
                hops[weight, piece, step] = copy
                sent.append(copy)
        for token in range(tokens):
            if step == ring - 2 - 2 * (tokens - 1 - token):
                rows[token, 1].wait_recv()
                send_rows(token, row_block(token, 2), 3, 2, peers[1])
    for weight in range(weights):
        for piece in range(QUAD):
            hops[weight, piece, ring - 2].wait_recv()
    for token in range(tokens):
        rows[token, 0].wait_recv()
        rows[token, 2].wait_recv()
    for copy in sent:
        copy.wait_send()
    for copy in kept:
        copy.wait()


def gather(identity, weight_list, token_list):
    ring = lax.axis_size("fs") // QUAD
    weights, tokens = len(weight_list), len(token_list)
    dma = pltpu.SemaphoreType.DMA
    outs = [
        jax.ShapeDtypeStruct((w.shape[0] * QUAD * ring, w.shape[1] // QUAD), w.dtype)
        for w in weight_list
    ] + [jax.ShapeDtypeStruct((t.shape[0] * QUAD, t.shape[1]), t.dtype) for t in token_list]
    return pl.pallas_call(
        functools.partial(gather_kernel, ring, weights, tokens),
        out_shape=outs,
        in_specs=[pl.BlockSpec(memory_space=pltpu.VMEM)] * (weights + tokens),
        out_specs=[pl.BlockSpec(memory_space=pl.ANY)] * (weights + tokens),
        scratch_shapes=[
            dma((weights, QUAD, ring - 1)),
            dma((weights, QUAD, ring - 1)),
            dma((weights, QUAD - 1)),
            dma((weights, QUAD - 1)),
            dma((tokens, 3)),
            dma((tokens, 3)),
            dma((weights + tokens,)),
        ],
        compiler_params=pltpu.CompilerParams(collective_id=identity, has_side_effects=True),
        cost_estimate=pl.CostEstimate(
            flops=0, bytes_accessed=weights * 90_000_000, transcendentals=0
        ),
    )(*weight_list, *token_list)


def quad_shards(
    later_input, earlier_input, cotangent, gate_weight, up_weight, down_weight, down_grad_sum
):
    total = lax.axis_size("fs")
    gate_whole, up_whole, early_rows, grad_rows = gather(
        0, (gate_weight, up_weight), (earlier_input, cotangent)
    )

    gate_early = jnp.dot(early_rows, gate_whole, preferred_element_type=jnp.float32)
    up_early = jnp.dot(early_rows, up_whole, preferred_element_type=jnp.float32)
    sigmoid_gate = jax.nn.sigmoid(gate_early)
    activated = gate_early * sigmoid_gate
    hidden_early = (activated * up_early).astype(jnp.bfloat16)
    partial_sum = lax.dot_general(
        grad_rows, hidden_early, (((0,), (0,)), ((), ())), preferred_element_type=jnp.float32
    ).astype(jnp.bfloat16)
    summed = lax.psum_scatter(
        partial_sum,
        "fs",
        scatter_dimension=0,
        tiled=True,
        axis_index_groups=lanes_of(total),
    )
    held_weight, held_input, _ = lax.optimization_barrier(
        (down_weight, later_input, partial_sum)
    )
    down_whole, later_rows = gather(1, (held_weight,), (held_input,))
    gate_later = jnp.dot(later_rows, gate_whole, preferred_element_type=jnp.float32)
    up_later = jnp.dot(later_rows, up_whole, preferred_element_type=jnp.float32)
    hidden_later = (jax.nn.silu(gate_later) * up_later).astype(jnp.bfloat16)

    grad_hidden = jnp.dot(grad_rows, down_whole, preferred_element_type=jnp.float32)
    grad_gate = (
        grad_hidden * up_early * sigmoid_gate * (1.0 + gate_early * (1.0 - sigmoid_gate))
    ).astype(jnp.bfloat16)
    grad_up = (grad_hidden * activated).astype(jnp.bfloat16)
    later_output = return_tokens(contract_last(hidden_later, down_whole))
    earlier_grad_input = return_tokens(
        contract_last(grad_gate, gate_whole) + contract_last(grad_up, up_whole)
    )
    own_rows = lax.all_to_all(
        summed, "fs", split_axis=0, concat_axis=1, tiled=True, axis_index_groups=quads_of(total)
    )
    factor = (later_input.shape[0] * total) ** (-0.5)
    return (
        later_output,
        earlier_grad_input,
        down_grad_sum + own_rows.astype(jnp.float32) * factor,
    )


def solution(mesh):
    in_specs = (
        P(("fs", "tp"), None),
        P(("fs", "tp"), None),
        P(("fs", "tp"), None),
        P("fs", "tp"),
        P("fs", "tp"),
        P("fs", "tp"),
        P("fs", "tp"),
    )
    out_specs = (P(("fs", "tp"), None), P(("fs", "tp"), None), P("fs", "tp"))
    split = mesh.shape["tp"] == 1 and mesh.shape["fs"] % (2 * QUAD) == 0
    body = quad_shards if split else shards
    return jax.shard_map(body, mesh=mesh, in_specs=in_specs, out_specs=out_specs, check_vma=False)
```

```python
import functools

import jax
import jax.numpy as jnp
from jax import lax
from jax.experimental import pallas as pl
from jax.experimental.pallas import tpu as pltpu
from jax.sharding import PartitionSpec as P

QUAD = 4


def contract_last(leading, trailing):
    return lax.dot_general(
        leading, trailing, (((1,), (1,)), ((), ())), preferred_element_type=jnp.float32
    )


def add_parts(received, group):
    pieces = received.reshape(group, received.shape[0] // group, received.shape[1])
    return jnp.sum(pieces.astype(jnp.float32), axis=0).astype(jnp.bfloat16)


def shards(
    later_input, earlier_input, cotangent, gate_weight, up_weight, down_weight, down_grad_sum
):
    group = lax.axis_size("tp")
    later_rows, early_rows, grad_rows = (
        lax.all_gather(later_input, "tp", axis=0, tiled=True),
        lax.all_gather(earlier_input, "tp", axis=0, tiled=True),
        lax.all_gather(cotangent, "tp", axis=0, tiled=True),
    )
    columns = later_rows
    gate_later = jnp.dot(
        columns,
        lax.all_gather(gate_weight, "fs", axis=0, tiled=True),
        preferred_element_type=jnp.float32,
    )
    up_later = jnp.dot(
        columns,
        lax.all_gather(up_weight, "fs", axis=0, tiled=True),
        preferred_element_type=jnp.float32,
    )
    hidden_later = (jax.nn.silu(gate_later) * up_later).astype(jnp.bfloat16)
    partials = contract_last(hidden_later, lax.all_gather(down_weight, "fs", axis=0, tiled=True))
    gate_whole, up_whole, down_whole = (
        lax.all_gather(gate_weight, "fs", axis=0, tiled=True),
        lax.all_gather(up_weight, "fs", axis=0, tiled=True),
        lax.all_gather(down_weight, "fs", axis=0, tiled=True),
    )
    output_received = lax.all_to_all(
        partials.astype(jnp.bfloat16), "tp", split_axis=0, concat_axis=0, tiled=True
    )
    later_output = add_parts(output_received, group)
    gate_early = jnp.dot(early_rows, gate_whole, preferred_element_type=jnp.float32)
    up_early = jnp.dot(early_rows, up_whole, preferred_element_type=jnp.float32)
    sigmoid_gate = jax.nn.sigmoid(gate_early)
    activated = gate_early * sigmoid_gate
    hidden_early = (activated * up_early).astype(jnp.bfloat16)
    grad_hidden = jnp.dot(grad_rows, down_whole, preferred_element_type=jnp.float32)
    grad_gate = (
        grad_hidden * up_early * sigmoid_gate * (1.0 + gate_early * (1.0 - sigmoid_gate))
    ).astype(jnp.bfloat16)
    grad_up = (grad_hidden * activated).astype(jnp.bfloat16)
    input_partial = contract_last(grad_gate, gate_whole) + contract_last(grad_up, up_whole)
    input_received = lax.all_to_all(
        input_partial.astype(jnp.bfloat16), "tp", split_axis=0, concat_axis=0, tiled=True
    )
    earlier_grad_input = add_parts(input_received, group)
    columns = grad_rows
    summed = lax.psum_scatter(
        lax.dot_general(
            columns, hidden_early, (((0,), (0,)), ((), ())), preferred_element_type=jnp.float32
        ),
        "fs",
        scatter_dimension=0,
        tiled=True,
    )
    factor = (later_rows.shape[0] * lax.axis_size("fs")) ** (-0.5)
    return (later_output, earlier_grad_input, down_grad_sum + summed * factor)

def quads_of(total):
    return [[first + place for place in range(QUAD)] for first in range(0, total, QUAD)]


def lanes_of(total):
    return [[first + place for first in range(0, total, QUAD)] for place in range(QUAD)]


def swap(value, bit):
    total = lax.axis_size("fs")
    return lax.ppermute(value, "fs", [(index, index ^ bit) for index in range(total)])


def return_tokens(partial):
    blocks = partial.astype(jnp.bfloat16).reshape(QUAD, -1, partial.shape[1])
    mine = partial.reshape(blocks.shape)
    near = swap(jnp.stack([blocks[1], blocks[3]]), 1).astype(jnp.float32)
    far = swap((mine[2] + near[1]).astype(jnp.bfloat16), 2)
    return (mine[0] + near[0] + far.astype(jnp.float32)).astype(jnp.bfloat16)

def ring_group(place, ring):
    half = lax.div(2 * place, ring)
    return 2 * place * (1 - half) + (2 * (ring - 1 - place) + 1) * half


def ring_place(group, ring):
    odd = lax.rem(group, 2)
    return lax.div(group, 2) * (1 - odd) + (ring - 1 - lax.div(group, 2)) * odd


def gather_kernel(ring, weights, tokens, *refs):
    weight_refs, token_refs = refs[:weights], refs[weights : weights + tokens]
    outs = refs[weights + tokens : 2 * (weights + tokens)]
    whole_refs, rows_refs = outs[:weights], outs[weights:]
    ring_send, ring_recv, quad_send, quad_recv, token_send, token_recv, local_sem = refs[
        2 * (weights + tokens) :
    ]
    me = lax.axis_index("fs")
    group, lane = lax.div(me, QUAD), lax.rem(me, QUAD)
    low, high = lax.rem(lane, 2), lax.div(lane, 2)
    relative = [lane, lane + 1 - 2 * low, lane + 2 - 4 * high, QUAD - 1 - lane]
    peers = [group * QUAD + other for other in relative]
    place = ring_place(group, ring)
    around = [
        ring_group(lax.rem(place + shift, ring), ring) * QUAD + lane for shift in (1, ring - 1)
    ]
    depth = weight_refs[0].shape[0]
    width = weight_refs[0].shape[1] // QUAD

    barrier = pltpu.get_barrier_semaphore()
    for other in peers[1:] + around:
        pl.semaphore_signal(
            barrier, inc=1, device_id={"fs": other}, device_id_type=pl.DeviceIdType.MESH
        )
    pl.semaphore_wait(barrier, QUAD + 1)

    def remote(source, target, send, recv, other):
        return pltpu.make_async_remote_copy(
            src_ref=source,
            dst_ref=target,
            send_sem=send,
            recv_sem=recv,
            device_id={"fs": other},
            device_id_type=pl.DeviceIdType.MESH,
        )

    def slab(weight, owner, member):
        first = pl.multiple_of((owner * QUAD + member) * depth, depth)
        return whole_refs[weight].at[pl.ds(first, depth), :]

    def columns(weight, member):
        return weight_refs[weight].at[:, pl.ds(pl.multiple_of(member * width, width), width)]

    sent, kept = [], []
    quad, hops, rows = {}, {}, {}
    for weight in range(weights):
        for far in (3, 2, 1):
            copy = remote(
                columns(weight, relative[far]),
                slab(weight, group, lane),
                quad_send.at[weight, far - 1],
                quad_recv.at[weight, far - 1],
                peers[far],
            )
            copy.start()
            quad[weight, far] = copy
            sent.append(copy)
    for weight in range(weights):
        copy = pltpu.make_async_copy(
            columns(weight, lane), slab(weight, group, lane), local_sem.at[weight]
        )
        copy.start()
        kept.append(copy)

    def row_block(token, block):
        count = token_refs[token].shape[0]
        return rows_refs[token].at[pl.ds(block * count, count), :]

    def send_rows(token, source, block, slot, other):
        copy = remote(
            source,
            row_block(token, block),
            token_send.at[token, slot],
            token_recv.at[token, slot],
            other,
        )
        copy.start()
        rows[token, slot] = copy
        sent.append(copy)

    for token in range(tokens):
        send_rows(token, token_refs[token], 2, 1, peers[2])
    for token in range(tokens):
        send_rows(token, token_refs[token], 1, 0, peers[1])
        copy = pltpu.make_async_copy(
            token_refs[token], row_block(token, 0), local_sem.at[weights + token]
        )
        copy.start()
        kept.append(copy)

    for step in range(ring - 1):
        for weight in range(weights):
            for piece in (0, 1, 3, 2):
                if step:
                    hops[weight, piece, step - 1].wait_recv()
                elif piece:
                    quad[weight, piece].wait_recv()
                forward = piece in (0, 3)
                back = ring - step if forward else step
                owner = ring_group(lax.rem(place + back, ring), ring)
                target = slab(weight, owner, relative[piece])
                copy = remote(
                    columns(weight, lane) if step == 0 and piece == 0 else target,
                    target,
                    ring_send.at[weight, piece, step],
                    ring_recv.at[weight, piece, step],
                    around[0 if forward else 1],
                )
                copy.start()
                hops[weight, piece, step] = copy
                sent.append(copy)
        for token in range(tokens):
            if step == ring - 2 - 2 * (tokens - 1 - token):
                rows[token, 1].wait_recv()
                send_rows(token, row_block(token, 2), 3, 2, peers[1])
    for weight in range(weights):
        for piece in range(QUAD):
            hops[weight, piece, ring - 2].wait_recv()
    for token in range(tokens):
        rows[token, 0].wait_recv()
        rows[token, 2].wait_recv()
    for copy in sent:
        copy.wait_send()
    for copy in kept:
        copy.wait()


def gather(identity, weight_list, token_list):
    ring = lax.axis_size("fs") // QUAD
    weights, tokens = len(weight_list), len(token_list)
    dma = pltpu.SemaphoreType.DMA
    outs = [
        jax.ShapeDtypeStruct((w.shape[0] * QUAD * ring, w.shape[1] // QUAD), w.dtype)
        for w in weight_list
    ] + [jax.ShapeDtypeStruct((t.shape[0] * QUAD, t.shape[1]), t.dtype) for t in token_list]
    return pl.pallas_call(
        functools.partial(gather_kernel, ring, weights, tokens),
        out_shape=outs,
        in_specs=[pl.BlockSpec(memory_space=pltpu.VMEM)] * (weights + tokens),
        out_specs=[pl.BlockSpec(memory_space=pl.ANY)] * (weights + tokens),
        scratch_shapes=[
            dma((weights, QUAD, ring - 1)),
            dma((weights, QUAD, ring - 1)),
            dma((weights, QUAD - 1)),
            dma((weights, QUAD - 1)),
            dma((tokens, 3)),
            dma((tokens, 3)),
            dma((weights + tokens,)),
        ],
        compiler_params=pltpu.CompilerParams(collective_id=identity, has_side_effects=True),
        cost_estimate=pl.CostEstimate(
            flops=0, bytes_accessed=weights * 90_000_000, transcendentals=0
        ),
    )(*weight_list, *token_list)


def quad_shards(
    later_input, earlier_input, cotangent, gate_weight, up_weight, down_weight, down_grad_sum
):
    total = lax.axis_size("fs")
    gate_whole, up_whole, down_whole, early_rows, grad_rows, later_rows = gather(
        0, (gate_weight, up_weight, down_weight), (earlier_input, cotangent, later_input)
    )

    gate_early = jnp.dot(early_rows, gate_whole, preferred_element_type=jnp.float32)
    up_early = jnp.dot(early_rows, up_whole, preferred_element_type=jnp.float32)
    sigmoid_gate = jax.nn.sigmoid(gate_early)
    activated = gate_early * sigmoid_gate
    hidden_early = (activated * up_early).astype(jnp.bfloat16)
    partial_sum = lax.dot_general(
        grad_rows, hidden_early, (((0,), (0,)), ((), ())), preferred_element_type=jnp.float32
    ).astype(jnp.bfloat16)
    summed = lax.psum_scatter(
        partial_sum,
        "fs",
        scatter_dimension=0,
        tiled=True,
        axis_index_groups=lanes_of(total),
    )
    down_whole, later_rows, _ = lax.optimization_barrier(
        (down_whole, later_rows, partial_sum)
    )
    gate_later = jnp.dot(later_rows, gate_whole, preferred_element_type=jnp.float32)
    up_later = jnp.dot(later_rows, up_whole, preferred_element_type=jnp.float32)
    hidden_later = (jax.nn.silu(gate_later) * up_later).astype(jnp.bfloat16)

    grad_hidden = jnp.dot(grad_rows, down_whole, preferred_element_type=jnp.float32)
    grad_gate = (
        grad_hidden * up_early * sigmoid_gate * (1.0 + gate_early * (1.0 - sigmoid_gate))
    ).astype(jnp.bfloat16)
    grad_up = (grad_hidden * activated).astype(jnp.bfloat16)
    later_output = return_tokens(contract_last(hidden_later, down_whole))
    earlier_grad_input = return_tokens(
        contract_last(grad_gate, gate_whole) + contract_last(grad_up, up_whole)
    )
    own_rows = lax.all_to_all(
        summed, "fs", split_axis=0, concat_axis=1, tiled=True, axis_index_groups=quads_of(total)
    )
    factor = (later_input.shape[0] * total) ** (-0.5)
    return (
        later_output,
        earlier_grad_input,
        down_grad_sum + own_rows.astype(jnp.float32) * factor,
    )


def solution(mesh):
    in_specs = (
        P(("fs", "tp"), None),
        P(("fs", "tp"), None),
        P(("fs", "tp"), None),
        P("fs", "tp"),
        P("fs", "tp"),
        P("fs", "tp"),
        P("fs", "tp"),
    )
    out_specs = (P(("fs", "tp"), None), P(("fs", "tp"), None), P("fs", "tp"))
    split = mesh.shape["tp"] == 1 and mesh.shape["fs"] % (2 * QUAD) == 0
    body = quad_shards if split else shards
    return jax.shard_map(body, mesh=mesh, in_specs=in_specs, out_specs=out_specs, check_vma=False)
```
